32 devices in a mesh: tp: 16 (over z, y, core), dp: 2 (over x).
Axes of the slice: x: 2, y: 2, z: 4, core: 2. Of those that a mesh axis runs over, the one named last changes fastest.
Arguments:
- resid: bfloat16 [64, 2048], P('dp', 'tp'), may hold values from -6 to 6
- norm_gain: float32 [2, 2048], replicated, may hold values from 0.1 to 1.9
- w_query: bfloat16 [2, 2048, 2048], P(None, 'dp', 'tp'), may hold values from -0.125 to 0.125
- w_forget: bfloat16 [2, 2048, 2048], P(None, 'dp', 'tp'), may hold values from -0.125 to 0.125
- w_value: bfloat16 [2, 2048, 16, 128], P(None, 'dp', None, 'tp'), may hold values from -0.125 to 0.125
- w_gate: bfloat16 [2, 2048, 16, 128], P(None, 'dp', None, 'tp'), may hold values from -0.125 to 0.125
- gate_floor: float32 [2, 2048], replicated, may hold values from 0 to 0.9
- states: float32 [2, 64, 16, 128, 128], P(None, 'dp', None, 'tp'), may hold values from -1 to 1
- out_gain: float32 [2, 16, 128], P(None, None, 'tp'), may hold values from 0.1 to 1.9
- w_out: bfloat16 [2, 16, 128, 2048], P(None, None, 'tp'), may hold values from -0.125 to 0.125
Outputs:
- new_resid: bfloat16 [64, 2048], P('dp', 'tp')
- new_states: float32 [2, 64, 16, 128, 128], P(None, 'dp', None, 'tp')
The draws below stay inside these ranges and needn't reach their ends.
All inputs are finite; a program needn't handle non-finite values.
Results may differ from the reference program's by a relative error of at most 0.029.
Values may be sent and summed in bfloat16 or wider, within the bound.
A program may use at most 64 MiB of HBM per device.

```python
import jax
import jax.numpy as jnp
from jax import lax

D = 2048
HEADS = 16
HD = 128
BLOCKS = 2
WIDTH = 2048
BATCH = 64
N_DP = 2


def block_scale(own_key, dims, split, low, largest):
    def one(axis_at, shards_of):
        heights = jax.random.uniform(jax.random.fold_in(jax.random.fold_in(own_key, 6), axis_at), (shards_of,), jnp.float32, low / len(split), largest / len(split))
        return jnp.repeat(jnp.exp(heights), dims[axis_at] // shards_of).reshape((-1,) + (1,) * (len(dims) - axis_at - 1))

    gain = one(*split[0])
    for cut in split[1:]:
        gain = gain * one(*cut)
    return gain


def normal_values(key, extent, deviation, bound, cuts=(), kind=jnp.bfloat16):
    values = jax.random.normal(key, extent, jnp.float32) * deviation
    if len(cuts) > 0:
        values = block_scale(key, extent, cuts, -0.22, 0.18) * values
    return jnp.clip(values, min=-bound, max=bound).astype(kind)


def setup_inputs(seed: int = 0) -> dict:
    key_of = jax.random.split(jax.random.key(seed), 11)
    return {
        "resid": normal_values(key_of[0], (BATCH, D), 1.0, 6.0, ((0, 2), (1, 16))),
        "norm_gain": jnp.clip(1.0 + 0.18 * jax.random.normal(key_of[1], (BLOCKS, D), jnp.float32), 0.1, 1.9),
        "w_query": normal_values(key_of[2], (BLOCKS, D, WIDTH), D ** -0.5, 0.125, ((1, 2), (2, 16))),
        "w_forget": normal_values(key_of[3], (BLOCKS, D, WIDTH), D ** -0.5, 0.125, ((1, 2), (2, 16))),
        "w_value": normal_values(key_of[4], (BLOCKS, D, HEADS, HD), D ** -0.5, 0.125, ((1, 2), (3, 16))),
        "w_gate": normal_values(key_of[5], (BLOCKS, D, HEADS, HD), D ** -0.5, 0.125, ((1, 2), (3, 16))),
        "gate_floor": jnp.clip(jax.random.uniform(key_of[6], (BLOCKS, WIDTH), jnp.float32, 0.0, 0.9), 0.0, 0.9),
        "states": normal_values(key_of[7], (BLOCKS, BATCH, HEADS, HD, HD), 0.15, 1.0, ((1, 2), (3, 16)), jnp.float32),
        "out_gain": jnp.clip(1.0 + 0.18 * jax.random.normal(key_of[8], (BLOCKS, HEADS, HD), jnp.float32), 0.1, 1.9),
        "w_out": normal_values(key_of[9], (BLOCKS, HEADS, HD, D), WIDTH ** -0.5, 0.125, ((2, 16),)),
    }


epsilon = 1e-06

def project(scaled, weight, inv_rms):
    row_count = weight.shape[0] // N_DP
    total = jnp.zeros((scaled.shape[0], weight.shape[1]), jnp.float32)
    for part_index in range(N_DP):
        lo_row = part_index * row_count
        partial_value = jnp.dot(scaled[:, lo_row:lo_row + row_count], weight[lo_row:lo_row + row_count], preferred_element_type=jnp.float32)
        total = total + lax.optimization_barrier(partial_value.astype(jnp.bfloat16)).astype(jnp.float32)
    return (total * inv_rms).astype(jnp.bfloat16)

def reference(resid, norm_gain, w_query, w_forget, w_value, w_gate, gate_floor, states, out_gain, w_out):
    residual = resid
    batch = resid.shape[0]
    new_list = []
    for layer in range(BLOCKS):
        resid_f32 = residual.astype(jnp.float32)
        inv_rms = lax.rsqrt(lax.optimization_barrier(jnp.mean(resid_f32 * resid_f32, axis=1, keepdims=True)) + epsilon)
        scaled = (resid_f32 * norm_gain[layer]).astype(jnp.bfloat16)
        queries = project(scaled, w_query[layer], inv_rms)
        forget_pre = project(scaled, w_forget[layer], inv_rms)
        values = project(scaled, w_value[layer].reshape(D, WIDTH), inv_rms)
        gate_pre = project(scaled, w_gate[layer].reshape(D, WIDTH), inv_rms)
        floor_now = gate_floor[layer]
        keep = floor_now + (1.0 - floor_now) * jax.nn.sigmoid(forget_pre.astype(jnp.float32))
        keep = keep.reshape(batch, HEADS, HD)
        value_f32 = values.astype(jnp.float32).reshape(batch, HEADS, HD)
        state_new = keep[:, :, None, :] * states[layer] + (1.0 - keep)[:, :, None, :] * value_f32[:, :, :, None]
        query_f32 = queries.astype(jnp.float32).reshape(batch, HEADS, HD)
        readout = lax.optimization_barrier(jnp.sum(query_f32[:, :, None, :] * state_new, axis=3))
        mean_square = lax.optimization_barrier(jnp.mean(readout * readout, axis=2, keepdims=True))
        gate_f32 = gate_pre.astype(jnp.float32).reshape(batch, HEADS, HD)
        normed = (readout * lax.rsqrt(mean_square + epsilon) * out_gain[layer] * jax.nn.silu(gate_f32)).astype(jnp.bfloat16)
        branch = jnp.dot(normed.reshape(batch, WIDTH), w_out[layer].reshape(WIDTH, D), preferred_element_type=jnp.float32)
        residual = (residual.astype(jnp.float32) + branch).astype(jnp.bfloat16)
        new_list.append(state_new)
    return (residual, jnp.stack(new_list))
```

```python
import functools

import jax
import jax.numpy as jnp
from jax import lax
from jax.experimental import pallas as pl
from jax.experimental.pallas import tpu as pltpu
from jax.sharding import PartitionSpec as P

BLOCKS = 2


epsilon = 1e-06


def shards(
    resid, norm_gain, w_query, w_forget, w_value, w_gate, gate_floor, states, out_gain, w_out
):
    residual = resid
    seq_local = resid.shape[0]
    heads = states.shape[2]
    slice_cols = states.shape[3]
    head_dim = states.shape[4]
    row_count = w_query.shape[1]
    new_list = []
    for layer in range(BLOCKS):
        gathered = lax.all_gather(residual, "tp", axis=1, tiled=True)
        resid_f32 = gathered.astype(jnp.float32)
        inv_rms = lax.rsqrt(jnp.mean(resid_f32 * resid_f32, axis=1, keepdims=True) + epsilon)
        scaled = (resid_f32 * norm_gain[layer]).astype(jnp.bfloat16)
        query_rows = w_query[layer]
        forget_rows = w_forget[layer]
        value_rows = w_value[layer].reshape(row_count, -1)
        gate_rows = w_gate[layer].reshape(row_count, -1)
        zero_sums = (
            jnp.zeros((seq_local, query_rows.shape[1]), jnp.float32),
            jnp.zeros((seq_local, forget_rows.shape[1]), jnp.float32),
            jnp.zeros((seq_local, value_rows.shape[1]), jnp.float32),
            jnp.zeros((seq_local, gate_rows.shape[1]), jnp.float32),
        )
        totals = zero_sums
        pieces = (
            lax.all_gather(query_rows, "dp", axis=0, tiled=True),
            lax.all_gather(forget_rows, "dp", axis=0, tiled=True),
            lax.all_gather(value_rows, "dp", axis=0, tiled=True),
            lax.all_gather(gate_rows, "dp", axis=0, tiled=True),
        )
        segments = pieces[0].shape[0] // row_count
        for part_index in range(segments):
            columns = lax.dynamic_slice_in_dim(scaled, part_index * row_count, row_count, 1)
            lo_row = part_index * row_count
            totals = tuple(
                (
                    total
                    + lax.optimization_barrier(
                        jnp.dot(
                            columns,
                            segment[lo_row : lo_row + row_count],
                            preferred_element_type=jnp.float32,
                        ).astype(jnp.bfloat16)
                    ).astype(jnp.float32)
                    for total, segment in zip(totals, pieces)
                )
            )
        queries, forget_pre, values, gate_pre = [
            (summed * inv_rms).astype(jnp.bfloat16) for summed in totals
        ]
        query_all, forget_all = (
            lax.all_gather(queries, "tp", axis=1, tiled=True),
            lax.all_gather(forget_pre, "tp", axis=1, tiled=True),
        )
        floor_now = gate_floor[layer]
        keep = floor_now + (1.0 - floor_now) * jax.nn.sigmoid(forget_all.astype(jnp.float32))
        keep = keep.reshape(seq_local, heads, head_dim)
        value_f32 = values.astype(jnp.float32).reshape(seq_local, heads, slice_cols)
        state_new = (
            keep[:, :, None, :] * states[layer]
            + (1.0 - keep)[:, :, None, :] * value_f32[:, :, :, None]
        )
        query_f32 = query_all.astype(jnp.float32).reshape(seq_local, heads, head_dim)
        readout = jnp.sum(query_f32[:, :, None, :] * state_new, axis=3)
        power_sum = lax.psum(jnp.sum(readout * readout, axis=2), "tp")
        mean_square = power_sum[..., None] / head_dim
        gate_f32 = gate_pre.astype(jnp.float32).reshape(seq_local, heads, slice_cols)
        normed = (
            readout * lax.rsqrt(mean_square + epsilon) * out_gain[layer] * jax.nn.silu(gate_f32)
        ).astype(jnp.bfloat16)
        flattened = normed.reshape(seq_local, heads * slice_cols)
        weight_out = w_out[layer].reshape(heads * slice_cols, -1)
        branch = lax.psum_scatter(
            lax.dot_general(
                weight_out, flattened, (((0,), (1,)), ((), ())), preferred_element_type=jnp.float32
            ),
            "tp",
            scatter_dimension=0,
            tiled=True,
        )
        residual = (residual.astype(jnp.float32) + branch.T).astype(jnp.bfloat16)
        new_list.append(state_new)
    return (residual, jnp.stack(new_list))


def fused_kernel(
    n_tp,
    n_dp,
    resid_ref,
    gain_ref,
    floor_ref,
    out_gain_ref,
    wq_hbm,
    wf_hbm,
    wv_hbm,
    wg_hbm,
    wo_hbm,
    states_hbm,
    resid_out,
    states_out,
    wq,
    wf,
    wv,
    wg,
    wo,
    st,
    x_own,
    x_all,
    scaled,
    part_out,
    part_in,
    ss_out,
    ss_in,
    qf_own,
    qf_all,
    q_f32,
    keep_f32,
    pw_own,
    pw_all,
    br_out,
    br_in,
    local_sem,
    state_in_sem,
    state_out_sem,
    x_send,
    x_recv,
    p_send,
    p_recv,
    s_send,
    s_recv,
    q_send,
    q_recv,
    w_send,
    w_recv,
    b_send,
    b_recv,
):
    me_t = lax.axis_index("tp")
    me_d = lax.axis_index("dp")
    seqs, cols = resid_ref.shape
    heads, slice_cols, head_dim = st.shape[2:]
    per_dp = n_tp // n_dp
    width = n_tp * cols
    blocks = wq.shape[0]
    bf16, f32 = jnp.bfloat16, jnp.float32

    weights = ((wq_hbm, wq), (wf_hbm, wf), (wv_hbm, wv), (wg_hbm, wg), (wo_hbm, wo))
    weight_copies = [
        [
            pltpu.make_async_copy(src.at[layer], dst.at[layer], local_sem.at[layer, i])
            for i, (src, dst) in enumerate(weights)
        ]
        for layer in range(blocks)
    ]
    state_copies = [
        pltpu.make_async_copy(states_hbm.at[layer], st.at[layer], state_in_sem.at[layer])
        for layer in range(blocks)
    ]

    barrier = pltpu.get_barrier_semaphore()

    def greet(k, carry):
        t = lax.rem(me_t + k // n_dp, n_tp)
        d = lax.rem(me_d + k % n_dp, n_dp)
        pl.semaphore_signal(barrier, inc=1, device_id={"tp": t, "dp": d})
        return carry

    lax.fori_loop(1, n_tp * n_dp, greet, 0)
    for layer in range(blocks):
        for copy in weight_copies[layer]:
            copy.start()
        state_copies[layer].start()
    x_own[0] = resid_ref[...]

    row_of = lax.broadcasted_iota(jnp.int32, (slice_cols, heads * slice_cols), 0)
    col_of = lax.broadcasted_iota(jnp.int32, (slice_cols, heads * slice_cols), 1)
    head_row = lax.broadcasted_iota(jnp.int32, (heads, heads * slice_cols), 0)
    head_col = lax.broadcasted_iota(jnp.int32, (heads, heads * slice_cols), 1)
    spread = (head_col // slice_cols == head_row).astype(f32)
    gains = []
    for layer in range(blocks):
        wide = jnp.dot(
            out_gain_ref[layer], spread, preferred_element_type=f32, precision=lax.Precision.HIGHEST
        )
        gains.append(
            jnp.sum(jnp.where(col_of % slice_cols == row_of, wide, 0.0), axis=0, keepdims=True)
        )

    pl.semaphore_wait(barrier, n_tp * n_dp - 1)

    group = seqs // 8
    lanes = 128 // group
    lane8 = lax.broadcasted_iota(jnp.int32, (8, 128), 1)
    state_lane = lax.broadcasted_iota(jnp.int32, (heads, slice_cols, 128), 2)

    for layer in range(blocks):
        x_d = me_t // per_dp
        x_j = me_t % per_dp

        def x_copy(k):
            return pltpu.make_async_remote_copy(
                src_ref=x_own.at[layer],
                dst_ref=x_all.at[layer, me_d, x_j],
                send_sem=x_send.at[layer, k],
                recv_sem=x_recv.at[layer, me_d, x_j],
                device_id={"tp": lax.rem(me_t + k, n_tp), "dp": x_d},
            )

        def x_start(k, carry):
            x_copy(k).start()
            return carry

        lax.fori_loop(1, n_tp, x_start, 0)

        @pl.when(x_d != me_d)
        def _():
            x_copy(0).start()

        @pl.when(x_d == me_d)
        def _():
            pltpu.make_async_copy(
                x_own.at[layer], x_all.at[layer, me_d, x_j], x_recv.at[layer, me_d, x_j]
            ).start()

        squares = []
        for d in range(n_dp):
            total = jnp.zeros((seqs, cols), f32)
            for j in range(per_dp):
                pltpu.make_async_copy(
                    x_own.at[layer], x_all.at[layer, d, j], x_recv.at[layer, d, j]
                ).wait()
                chunk = x_all[layer, d, j].astype(f32)
                total = total + chunk * chunk
                start = pl.multiple_of((me_d * per_dp + j) * cols, cols)
                scaled[d * seqs : (d + 1) * seqs, j * cols : (j + 1) * cols] = (
                    chunk * gain_ref[layer : layer + 1, pl.ds(start, cols)]
                ).astype(bf16)
            squares.append(jnp.sum(total, axis=1, keepdims=True))

        for copy in weight_copies[layer]:
            copy.wait()
        xs = scaled[...]
        nt = (((1,), (1,)), ((), ()))
        parts = (
            jnp.dot(xs, wq[layer], preferred_element_type=f32),
            jnp.dot(xs, wf[layer], preferred_element_type=f32),
            lax.dot_general(xs, wv[layer], nt, preferred_element_type=f32),
            lax.dot_general(xs, wg[layer], nt, preferred_element_type=f32),
        )
        for d in range(n_dp):
            for i in range(4):
                part_out[layer, d, i] = parts[i][d * seqs : (d + 1) * seqs].astype(bf16)
            tile = jnp.zeros((8, 128), f32)
            for g in range(group):
                tile = jnp.where(lane8 // lanes == g, squares[d][g * 8 : (g + 1) * 8], tile)
            ss_out[layer, d] = tile

        def p_copies(k):
            peer = lax.rem(me_d + k, n_dp)
            to = {"tp": me_t, "dp": peer}
            return (
                pltpu.make_async_remote_copy(
                    src_ref=part_out.at[layer, peer],
                    dst_ref=part_in.at[layer, me_d],
                    send_sem=p_send.at[layer, k],
                    recv_sem=p_recv.at[layer, me_d],
                    device_id=to,
                ),
                pltpu.make_async_remote_copy(
                    src_ref=ss_out.at[layer, peer],
                    dst_ref=ss_in.at[layer, me_d],
                    send_sem=s_send.at[layer, k],
                    recv_sem=s_recv.at[layer, me_d],
                    device_id=to,
                ),
            )

        for k in range(1, n_dp):
            for copy in p_copies(k):
                copy.start()
        sums = [part_out[layer, me_d, i].astype(f32) for i in range(4)]
        square_tile = ss_out[layer, me_d]
        for k in range(1, n_dp):
            src = lax.rem(me_d + k, n_dp)
            pltpu.make_async_copy(
                part_out.at[layer, src], part_in.at[layer, src], p_recv.at[layer, src]
            ).wait()
            pltpu.make_async_copy(
                ss_out.at[layer, src], ss_in.at[layer, src], s_recv.at[layer, src]
            ).wait()
            sums = [sums[i] + part_in[layer, src, i].astype(f32) for i in range(4)]
            square_tile = square_tile + ss_in[layer, src]
        inv_tile = lax.rsqrt(square_tile / width + epsilon)
        inv_rms = jnp.concatenate(
            [inv_tile[:, g * lanes : g * lanes + 1] for g in range(group)], axis=0
        )
        query, forget, value, gate = [(s * inv_rms).astype(bf16) for s in sums]
        qf_own[layer, 0] = query
        qf_own[layer, 1] = forget

        def q_copy(k):
            return pltpu.make_async_remote_copy(
                src_ref=qf_own.at[layer],
                dst_ref=qf_all.at[layer, me_t],
                send_sem=q_send.at[layer, k],
                recv_sem=q_recv.at[layer, me_t],
                device_id={"tp": lax.rem(me_t + k, n_tp), "dp": me_d},
            )

        def q_start(k, carry):
            q_copy(k).start()
            return carry

        lax.fori_loop(1, n_tp, q_start, 0)
        qf_all[layer, me_t] = qf_own[layer]

        value_t = jnp.transpose(
            jnp.concatenate(
                [value.astype(f32), jnp.zeros((128 - seqs, value.shape[1]), f32)], axis=0
            )
        ).reshape(heads, slice_cols, 128)
        gate_f32 = gate.astype(f32)
        gated = gains[layer] * (gate_f32 / (1.0 + jnp.exp(-gate_f32)))

        def q_wait(k, carry):
            src = lax.rem(me_t + n_tp - k, n_tp)
            pltpu.make_async_copy(
                qf_own.at[layer], qf_all.at[layer, src], q_recv.at[layer, src]
            ).wait()
            return carry

        lax.fori_loop(1, n_tp, q_wait, 0)
        for h in range(heads):
            floor_now = floor_ref[layer : layer + 1, h * head_dim : (h + 1) * head_dim]
            q_f32[h] = qf_all[layer, h, 0].astype(f32)
            keep_f32[h] = floor_now + (1.0 - floor_now) * jax.nn.sigmoid(
                qf_all[layer, h, 1].astype(f32)
            )
        state_copies[layer].wait()
        readout = jnp.zeros((heads, slice_cols, 128), f32)
        for s in range(seqs):
            keep = keep_f32[:, s : s + 1, :]
            new = keep * st[layer, s] + (1.0 - keep) * value_t[:, :, s : s + 1]
            st[layer, s] = new
            summed = jnp.sum(q_f32[:, s : s + 1, :] * new, axis=2, keepdims=True)
            readout = jnp.where(state_lane == s, summed, readout)
        pltpu.make_async_copy(st.at[layer], states_out.at[layer], state_out_sem.at[layer]).start()

        power = jnp.sum(readout * readout, axis=1)
        pw_own[layer] = power

        def w_copy(k):
            return pltpu.make_async_remote_copy(
                src_ref=pw_own.at[layer],
                dst_ref=pw_all.at[layer, me_t],
                send_sem=w_send.at[layer, k],
                recv_sem=w_recv.at[layer, me_t],
                device_id={"tp": lax.rem(me_t + k, n_tp), "dp": me_d},
            )

        def w_start(k, carry):
            w_copy(k).start()
            return carry

        lax.fori_loop(1, n_tp, w_start, 0)
        pw_all[layer, me_t] = power

        def w_wait(k, carry):
            src = lax.rem(me_t + n_tp - k, n_tp)
            pltpu.make_async_copy(
                pw_own.at[layer], pw_all.at[layer, src], w_recv.at[layer, src]
            ).wait()
            return carry

        lax.fori_loop(1, n_tp, w_wait, 0)
        mean_square = jnp.sum(pw_all[layer], axis=0) / head_dim
        unit = readout * lax.rsqrt(mean_square + epsilon)[:, None, :]
        unit = jnp.transpose(unit.reshape(heads * slice_cols, 128))[:seqs]
        normed = (unit * gated).astype(bf16)
        for t in range(n_tp):
            br_out[layer, t] = jnp.dot(
                normed, wo[layer, :, t * cols : (t + 1) * cols], preferred_element_type=f32
            ).astype(bf16)

        def b_copy(k):
            to = lax.rem(me_t + k, n_tp)
            return pltpu.make_async_remote_copy(
                src_ref=br_out.at[layer, to],
                dst_ref=br_in.at[layer, me_t],
                send_sem=b_send.at[layer, k],
                recv_sem=b_recv.at[layer, me_t],
                device_id={"tp": to, "dp": me_d},
            )

        def b_start(k, carry):
            b_copy(k).start()
            return carry

        lax.fori_loop(1, n_tp, b_start, 0)
        br_in[layer, me_t] = br_out[layer, me_t]

        def b_wait(k, carry):
            src = lax.rem(me_t + n_tp - k, n_tp)
            pltpu.make_async_copy(
                br_out.at[layer, src], br_in.at[layer, src], b_recv.at[layer, src]
            ).wait()
            return carry

        lax.fori_loop(1, n_tp, b_wait, 0)
        branch = jnp.sum(br_in[layer].astype(f32), axis=0)
        new_resid = (x_own[layer].astype(f32) + branch).astype(bf16)
        if layer + 1 < blocks:
            x_own[layer + 1] = new_resid
        else:
            resid_out[...] = new_resid

        @pl.when(x_d != me_d)
        def _():
            x_copy(0).wait_send()

        def drain(k, carry):
            x_copy(k).wait_send()
            q_copy(k).wait_send()
            w_copy(k).wait_send()
            b_copy(k).wait_send()
            return carry

        lax.fori_loop(1, n_tp, drain, 0)
        for k in range(1, n_dp):
            for copy in p_copies(k):
                copy.wait_send()

    for layer in range(blocks):
        pltpu.make_async_copy(st.at[layer], states_out.at[layer], state_out_sem.at[layer]).wait()


def fused_shards(
    n_tp,
    n_dp,
    resid,
    norm_gain,
    w_query,
    w_forget,
    w_value,
    w_gate,
    gate_floor,
    states,
    out_gain,
    w_out,
):
    seqs, cols = resid.shape
    blocks, _, heads, slice_cols, head_dim = states.shape
    rows = w_query.shape[1]
    local = heads * slice_cols
    width = w_out.shape[3]
    value_t = jnp.transpose(w_value, (0, 2, 3, 1)).reshape(blocks, local, rows)
    gate_t = jnp.transpose(w_gate, (0, 2, 3, 1)).reshape(blocks, local, rows)
    bf16, f32 = jnp.bfloat16, jnp.float32
    dma = pltpu.SemaphoreType.DMA
    vmem = pl.BlockSpec(memory_space=pltpu.VMEM)
    hbm = pl.BlockSpec(memory_space=pl.ANY)
    per_dp = n_tp // n_dp
    return pl.pallas_call(
        functools.partial(fused_kernel, n_tp, n_dp),
        out_shape=(
            jax.ShapeDtypeStruct(resid.shape, resid.dtype),
            jax.ShapeDtypeStruct(states.shape, states.dtype),
        ),
        in_specs=[vmem] * 4 + [hbm] * 6,
        out_specs=(vmem, hbm),
        scratch_shapes=[
            pltpu.VMEM(w_query.shape, bf16),
            pltpu.VMEM(w_forget.shape, bf16),
            pltpu.VMEM(value_t.shape, bf16),
            pltpu.VMEM(gate_t.shape, bf16),
            pltpu.VMEM((blocks, local, width), bf16),
            pltpu.VMEM(states.shape, f32),
            pltpu.VMEM((blocks, seqs, cols), bf16),
            pltpu.VMEM((blocks, n_dp, per_dp, seqs, cols), bf16),
            pltpu.VMEM((n_dp * seqs, rows), bf16),
            pltpu.VMEM((blocks, n_dp, 4, seqs, cols), bf16),
            pltpu.VMEM((blocks, n_dp, 4, seqs, cols), bf16),
            pltpu.VMEM((blocks, n_dp, 8, 128), f32),
            pltpu.VMEM((blocks, n_dp, 8, 128), f32),
            pltpu.VMEM((blocks, 2, seqs, cols), bf16),
            pltpu.VMEM((blocks, n_tp, 2, seqs, cols), bf16),
            pltpu.VMEM((heads, seqs, head_dim), f32),
            pltpu.VMEM((heads, seqs, head_dim), f32),
            pltpu.VMEM((blocks, heads, 128), f32),
            pltpu.VMEM((blocks, n_tp, heads, 128), f32),
            pltpu.VMEM((blocks, n_tp, seqs, cols), bf16),
            pltpu.VMEM((blocks, n_tp, seqs, cols), bf16),
            dma((blocks, 5)),
            dma((blocks,)),
            dma((blocks,)),
            dma((blocks, n_tp)),
            dma((blocks, n_dp, per_dp)),
            dma((blocks, n_dp)),
            dma((blocks, n_dp)),
            dma((blocks, n_dp)),
            dma((blocks, n_dp)),
            dma((blocks, n_tp)),
            dma((blocks, n_tp)),
            dma((blocks, n_tp)),
            dma((blocks, n_tp)),
            dma((blocks, n_tp)),
            dma((blocks, n_tp)),
        ],
        compiler_params=pltpu.CompilerParams(
            collective_id=0, has_side_effects=True, vmem_limit_bytes=56 * 1024 * 1024
        ),
    )(
        resid,
        norm_gain,
        gate_floor,
        jnp.transpose(out_gain, (0, 2, 1)),
        w_query,
        w_forget,
        value_t,
        gate_t,
        w_out.reshape(blocks, local, width),
        states,
    )


def choose(n_tp, n_dp, *args):
    resid, w_query, states = args[0], args[2], args[7]
    seqs, cols = resid.shape
    _, _, heads, slice_cols, head_dim = states.shape
    whole_tiles = (
        cols == 128
        and head_dim == 128
        and heads == n_tp
        and slice_cols == 8
        and w_query.shape[2] == cols
        and heads * slice_cols == cols
        and n_tp % n_dp == 0
        and seqs % 16 == 0
        and seqs <= 128
        and 1024 % seqs == 0
    )
    body = functools.partial(fused_shards, n_tp, n_dp) if whole_tiles else shards
    return body(*args)


def solution(mesh):
    return jax.shard_map(
        functools.partial(choose, mesh.shape["tp"], mesh.shape["dp"]),
        mesh=mesh,
        in_specs=(
            P("dp", "tp"),
            P(),
            P(None, "dp", "tp"),
            P(None, "dp", "tp"),
            P(None, "dp", None, "tp"),
            P(None, "dp", None, "tp"),
            P(),
            P(None, "dp", None, "tp", None),
            P(None, None, "tp"),
            P(None, None, "tp", None),
        ),
        out_specs=(P("dp", "tp"), P(None, "dp", None, "tp", None)),
        check_vma=False,
    )
```

```python
import functools

import jax
import jax.numpy as jnp
from jax import lax
from jax.experimental import pallas as pl
from jax.experimental.pallas import tpu as pltpu
from jax.sharding import PartitionSpec as P

BLOCKS = 2


epsilon = 1e-06


def shards(
    resid, norm_gain, w_query, w_forget, w_value, w_gate, gate_floor, states, out_gain, w_out
):
    residual = resid
    seq_local = resid.shape[0]
    heads = states.shape[2]
    slice_cols = states.shape[3]
    head_dim = states.shape[4]
    row_count = w_query.shape[1]
    new_list = []
    for layer in range(BLOCKS):
        gathered = lax.all_gather(residual, "tp", axis=1, tiled=True)
        resid_f32 = gathered.astype(jnp.float32)
        inv_rms = lax.rsqrt(jnp.mean(resid_f32 * resid_f32, axis=1, keepdims=True) + epsilon)
        scaled = (resid_f32 * norm_gain[layer]).astype(jnp.bfloat16)
        query_rows = w_query[layer]
        forget_rows = w_forget[layer]
        value_rows = w_value[layer].reshape(row_count, -1)
        gate_rows = w_gate[layer].reshape(row_count, -1)
        zero_sums = (
            jnp.zeros((seq_local, query_rows.shape[1]), jnp.float32),
            jnp.zeros((seq_local, forget_rows.shape[1]), jnp.float32),
            jnp.zeros((seq_local, value_rows.shape[1]), jnp.float32),
            jnp.zeros((seq_local, gate_rows.shape[1]), jnp.float32),
        )
        totals = zero_sums
        pieces = (
            lax.all_gather(query_rows, "dp", axis=0, tiled=True),
            lax.all_gather(forget_rows, "dp", axis=0, tiled=True),
            lax.all_gather(value_rows, "dp", axis=0, tiled=True),
            lax.all_gather(gate_rows, "dp", axis=0, tiled=True),
        )
        segments = pieces[0].shape[0] // row_count
        for part_index in range(segments):
            columns = lax.dynamic_slice_in_dim(scaled, part_index * row_count, row_count, 1)
            lo_row = part_index * row_count
            totals = tuple(
                (
                    total
                    + lax.optimization_barrier(
                        jnp.dot(
                            columns,
                            segment[lo_row : lo_row + row_count],
                            preferred_element_type=jnp.float32,
                        ).astype(jnp.bfloat16)
                    ).astype(jnp.float32)
                    for total, segment in zip(totals, pieces)
                )
            )
        queries, forget_pre, values, gate_pre = [
            (summed * inv_rms).astype(jnp.bfloat16) for summed in totals
        ]
        query_all, forget_all = (
            lax.all_gather(queries, "tp", axis=1, tiled=True),
            lax.all_gather(forget_pre, "tp", axis=1, tiled=True),
        )
        floor_now = gate_floor[layer]
        keep = floor_now + (1.0 - floor_now) * jax.nn.sigmoid(forget_all.astype(jnp.float32))
        keep = keep.reshape(seq_local, heads, head_dim)
        value_f32 = values.astype(jnp.float32).reshape(seq_local, heads, slice_cols)
        state_new = (
            keep[:, :, None, :] * states[layer]
            + (1.0 - keep)[:, :, None, :] * value_f32[:, :, :, None]
        )
        query_f32 = query_all.astype(jnp.float32).reshape(seq_local, heads, head_dim)
        readout = jnp.sum(query_f32[:, :, None, :] * state_new, axis=3)
        power_sum = lax.psum(jnp.sum(readout * readout, axis=2), "tp")
        mean_square = power_sum[..., None] / head_dim
        gate_f32 = gate_pre.astype(jnp.float32).reshape(seq_local, heads, slice_cols)
        normed = (
            readout * lax.rsqrt(mean_square + epsilon) * out_gain[layer] * jax.nn.silu(gate_f32)
        ).astype(jnp.bfloat16)
        flattened = normed.reshape(seq_local, heads * slice_cols)
        weight_out = w_out[layer].reshape(heads * slice_cols, -1)
        branch = lax.psum_scatter(
            lax.dot_general(
                weight_out, flattened, (((0,), (1,)), ((), ())), preferred_element_type=jnp.float32
            ),
            "tp",
            scatter_dimension=0,
            tiled=True,
        )
        residual = (residual.astype(jnp.float32) + branch.T).astype(jnp.bfloat16)
        new_list.append(state_new)
    return (residual, jnp.stack(new_list))


def fused_kernel(
    n_tp,
    n_dp,
    resid_ref,
    gain_ref,
    floor_ref,
    out_gain_ref,
    wq_hbm,
    wf_hbm,
    wv_hbm,
    wg_hbm,
    wo_hbm,
    states_hbm,
    resid_out,
    st,
    wq,
    wf,
    wv,
    wg,
    wo,
    x_own,
    x_all,
    scaled,
    part_out,
    part_in,
    ss_out,
    ss_in,
    qf_own,
    qf_all,
    q_f32,
    keep_f32,
    v_cols,
    reads,
    pw_own,
    pw_all,
    br_out,
    br_in,
    local_sem,
    state_in_sem,
    x_send,
    x_recv,
    p_send,
    p_recv,
    s_send,
    s_recv,
    q_send,
    q_recv,
    w_send,
    w_recv,
    b_send,
    b_recv,
):
    me_t = lax.axis_index("tp")
    me_d = lax.axis_index("dp")
    seqs, cols = resid_ref.shape
    heads, slice_cols, head_dim = st.shape[2:]
    per_dp = n_tp // n_dp
    width = n_tp * cols
    blocks = wq.shape[0]
    bf16, f32 = jnp.bfloat16, jnp.float32

    weights = ((wq_hbm, wq), (wf_hbm, wf), (wv_hbm, wv), (wg_hbm, wg), (wo_hbm, wo))
    weight_copies = [
        [
            pltpu.make_async_copy(src.at[layer], dst.at[layer], local_sem.at[layer, i])
            for i, (src, dst) in enumerate(weights)
        ]
        for layer in range(blocks)
    ]
    state_copies = [
        pltpu.make_async_copy(states_hbm.at[layer], st.at[layer], state_in_sem.at[layer])
        for layer in range(blocks)
    ]

    barrier = pltpu.get_barrier_semaphore()

    def greet(k, carry):
        t = lax.rem(me_t + k // n_dp, n_tp)
        d = lax.rem(me_d + k % n_dp, n_dp)
        pl.semaphore_signal(barrier, inc=1, device_id={"tp": t, "dp": d})
        return carry

    lax.fori_loop(1, n_tp * n_dp, greet, 0)
    for layer in range(blocks):
        for copy in weight_copies[layer]:
            copy.start()
        state_copies[layer].start()
    x_own[0] = resid_ref[...]

    row_of = lax.broadcasted_iota(jnp.int32, (slice_cols, heads * slice_cols), 0)
    col_of = lax.broadcasted_iota(jnp.int32, (slice_cols, heads * slice_cols), 1)
    head_row = lax.broadcasted_iota(jnp.int32, (heads, heads * slice_cols), 0)
    head_col = lax.broadcasted_iota(jnp.int32, (heads, heads * slice_cols), 1)
    spread = (head_col // slice_cols == head_row).astype(f32)
    gains = []
    for layer in range(blocks):
        wide = jnp.dot(
            out_gain_ref[layer], spread, preferred_element_type=f32, precision=lax.Precision.HIGHEST
        )
        gains.append(
            jnp.sum(jnp.where(col_of % slice_cols == row_of, wide, 0.0), axis=0, keepdims=True)
        )

    pl.semaphore_wait(barrier, n_tp * n_dp - 1)

    group = seqs // 8
    lanes = 128 // group
    lane8 = lax.broadcasted_iota(jnp.int32, (8, 128), 1)
    row_lane = lax.broadcasted_iota(jnp.int32, (slice_cols, 128), 1)
    heads_deep = heads * seqs // 128

    def sent(sem, like):
        pltpu.make_async_copy(like, like, sem).wait()

    for layer in range(blocks):
        x_d = me_t // per_dp
        x_j = me_t % per_dp

        def x_copy(k):
            return pltpu.make_async_remote_copy(
                src_ref=x_own.at[layer],
                dst_ref=x_all.at[layer, me_d, x_j],
                send_sem=x_send.at[layer],
                recv_sem=x_recv.at[layer, me_d, x_j],
                device_id={"tp": lax.rem(me_t + k, n_tp), "dp": x_d},
            )

        for k in range(1, n_tp):
            x_copy(k).start()

        @pl.when(x_d != me_d)
        def _():
            x_copy(0).start()

        @pl.when(x_d == me_d)
        def _():
            pltpu.make_async_copy(
                x_own.at[layer], x_all.at[layer, me_d, x_j], x_recv.at[layer, me_d, x_j]
            ).start()

        if layer > 0:
            sent(b_send.at[layer - 1], br_out.at[layer - 1, 1:])
        squares = []
        for d in range(n_dp):
            total = jnp.zeros((seqs, cols), f32)
            for j in range(per_dp):
                pltpu.make_async_copy(
                    x_own.at[layer], x_all.at[layer, d, j], x_recv.at[layer, d, j]
                ).wait()
                chunk = x_all[layer, d, j].astype(f32)
                total = total + chunk * chunk
                start = pl.multiple_of((me_d * per_dp + j) * cols, cols)
                scaled[d * seqs : (d + 1) * seqs, j * cols : (j + 1) * cols] = (
                    chunk * gain_ref[layer : layer + 1, pl.ds(start, cols)]
                ).astype(bf16)
            squares.append(jnp.sum(total, axis=1, keepdims=True))

        for copy in weight_copies[layer]:
            copy.wait()
        xs = scaled[...]
        nt = (((1,), (1,)), ((), ()))
        parts = (
            jnp.dot(xs, wq[layer], preferred_element_type=f32),
            jnp.dot(xs, wf[layer], preferred_element_type=f32),
            lax.dot_general(xs, wv[layer], nt, preferred_element_type=f32),
            lax.dot_general(xs, wg[layer], nt, preferred_element_type=f32),
        )
        for d in range(n_dp):
            for i in range(4):
                part_out[layer, d, i] = parts[i][d * seqs : (d + 1) * seqs].astype(bf16)
            tile = jnp.zeros((8, 128), f32)
            for g in range(group):
                tile = jnp.where(lane8 // lanes == g, squares[d][g * 8 : (g + 1) * 8], tile)
            ss_out[layer, d] = tile

        def p_copies(k):
            peer = lax.rem(me_d + k, n_dp)
            to = {"tp": me_t, "dp": peer}
            return (
                pltpu.make_async_remote_copy(
                    src_ref=part_out.at[layer, peer],
                    dst_ref=part_in.at[layer, me_d],
                    send_sem=p_send.at[layer, k],
                    recv_sem=p_recv.at[layer, me_d],
                    device_id=to,
                ),
                pltpu.make_async_remote_copy(
                    src_ref=ss_out.at[layer, peer],
                    dst_ref=ss_in.at[layer, me_d],
                    send_sem=s_send.at[layer, k],
                    recv_sem=s_recv.at[layer, me_d],
                    device_id=to,
                ),
            )

        for k in range(1, n_dp):
            for copy in p_copies(k):
                copy.start()
        sums = [part_out[layer, me_d, i].astype(f32) for i in range(4)]
        square_tile = ss_out[layer, me_d]
        for k in range(1, n_dp):
            src = lax.rem(me_d + k, n_dp)
            pltpu.make_async_copy(
                part_out.at[layer, src], part_in.at[layer, src], p_recv.at[layer, src]
            ).wait()
            pltpu.make_async_copy(
                ss_out.at[layer, src], ss_in.at[layer, src], s_recv.at[layer, src]
            ).wait()
            sums = [sums[i] + part_in[layer, src, i].astype(f32) for i in range(4)]
            square_tile = square_tile + ss_in[layer, src]
        inv_tile = lax.rsqrt(square_tile / width + epsilon)
        inv_rms = jnp.concatenate(
            [inv_tile[:, g * lanes : g * lanes + 1] for g in range(group)], axis=0
        )
        query, forget, value, gate = [(s * inv_rms).astype(bf16) for s in sums]
        qf_own[layer, 0] = query
        qf_own[layer, 1] = forget

        def q_copy(k):
            return pltpu.make_async_remote_copy(
                src_ref=qf_own.at[layer],
                dst_ref=qf_all.at[layer, me_t],
                send_sem=q_send.at[layer],
                recv_sem=q_recv.at[layer, me_t],
                device_id={"tp": lax.rem(me_t + k, n_tp), "dp": me_d},
            )

        for k in range(1, n_tp):
            q_copy(k).start()
        qf_all[layer, me_t] = qf_own[layer]

        value_t = jnp.transpose(
            jnp.concatenate(
                [value.astype(f32), jnp.zeros((128 - seqs, value.shape[1]), f32)], axis=0
            )
        ).reshape(heads, slice_cols, 128)
        gate_f32 = gate.astype(f32)
        gated = gains[layer] * (gate_f32 / (1.0 + jnp.exp(-gate_f32)))

        sent(x_send.at[layer], br_out.at[layer, 1:])

        @pl.when(x_d != me_d)
        def _():
            sent(x_send.at[layer], br_out.at[layer, 0])

        for k in range(1, n_dp):
            for copy in p_copies(k):
                copy.wait_send()
        v_cols[...] = value_t
        state_copies[layer].wait()

        def one_head(h):
            start = pl.multiple_of(h * head_dim, head_dim)
            floor_now = floor_ref[layer : layer + 1, pl.ds(start, head_dim)]
            q_f32[h] = qf_all[layer, h, 0].astype(f32)
            keep_f32[h] = floor_now + (1.0 - floor_now) * jax.nn.sigmoid(
                qf_all[layer, h, 1].astype(f32)
            )
            values_h = v_cols[h]
            first = (h // heads_deep) * seqs
            total = jnp.zeros((slice_cols, 128), f32)
            for base in range(0, seqs, 8):
                span = range(base, base + 8)
                olds = [st[layer, s, h] for s in span]
                keeps = [keep_f32[h, s : s + 1, :] for s in span]
                queries = [q_f32[h, s : s + 1, :] for s in span]
                news = [
                    keeps[i] * olds[i] + (1.0 - keeps[i]) * values_h[:, s : s + 1]
                    for i, s in enumerate(span)
                ]
                sums_h = [
                    jnp.sum(queries[i] * news[i], axis=1, keepdims=True) for i in range(8)
                ]
                for i, s in enumerate(span):
                    st[layer, s, h] = news[i]
                    total = jnp.where(row_lane == first + s, sums_h[i], total)
            reads[h] = total

        one_head(me_t)

        def far_head(k, carry):
            src = lax.rem(me_t + n_tp - k, n_tp)
            pltpu.make_async_copy(
                qf_own.at[layer], qf_all.at[layer, src], q_recv.at[layer, src]
            ).wait()
            one_head(src)
            return carry

        lax.fori_loop(1, n_tp, far_head, 0)
        readout = reads[...]
        power = jnp.sum(
            jnp.sum(readout * readout, axis=1).reshape(heads // heads_deep, heads_deep, 128), axis=0
        )
        pw_own[layer] = power

        def w_copy(k):
            return pltpu.make_async_remote_copy(
                src_ref=pw_own.at[layer],
                dst_ref=pw_all.at[layer, me_t],
                send_sem=w_send.at[layer],
                recv_sem=w_recv.at[layer],
                device_id={"tp": lax.rem(me_t + k, n_tp), "dp": me_d},
            )

        for k in range(1, n_tp):
            w_copy(k).start()
        pw_all[layer, me_t] = power

        sent(q_send.at[layer], qf_all.at[layer, 1:])
        pltpu.make_async_copy(
            pw_all.at[layer, 1:], pw_all.at[layer, 1:], w_recv.at[layer]
        ).wait()
        mean_square = jnp.sum(pw_all[layer], axis=0) / head_dim
        folds = heads // heads_deep
        unit = (
            readout.reshape(folds, heads_deep, slice_cols, 128)
            * lax.rsqrt(mean_square + epsilon)[None, :, None, :]
        )
        unit = jnp.transpose(unit.reshape(heads * slice_cols, 128))
        unit = jnp.sum(unit.reshape(folds, seqs, heads * slice_cols), axis=0)
        normed = (unit * gated).astype(bf16)
        for t in range(n_tp):
            br_out[layer, t] = jnp.dot(
                normed, wo[layer, :, t * cols : (t + 1) * cols], preferred_element_type=f32
            ).astype(bf16)

        def b_copy(k):
            to = lax.rem(me_t + k, n_tp)
            return pltpu.make_async_remote_copy(
                src_ref=br_out.at[layer, to],
                dst_ref=br_in.at[layer, me_t],
                send_sem=b_send.at[layer],
                recv_sem=b_recv.at[layer],
                device_id={"tp": to, "dp": me_d},
            )

        for k in range(1, n_tp):
            b_copy(k).start()
        br_in[layer, me_t] = br_out[layer, me_t]

        sent(w_send.at[layer], pw_all.at[layer, 1:])
        pltpu.make_async_copy(
            br_in.at[layer, 1:], br_in.at[layer, 1:], b_recv.at[layer]
        ).wait()
        branch = jnp.sum(br_in[layer].astype(f32), axis=0)
        new_resid = (x_own[layer].astype(f32) + branch).astype(bf16)
        if layer + 1 < blocks:
            x_own[layer + 1] = new_resid
        else:
            resid_out[...] = new_resid

    sent(b_send.at[blocks - 1], br_out.at[blocks - 1, 1:])


def fused_shards(
    n_tp,
    n_dp,
    resid,
    norm_gain,
    w_query,
    w_forget,
    w_value,
    w_gate,
    gate_floor,
    states,
    out_gain,
    w_out,
):
    seqs, cols = resid.shape
    blocks, _, heads, slice_cols, head_dim = states.shape
    rows = w_query.shape[1]
    local = heads * slice_cols
    width = w_out.shape[3]
    value_t = jnp.transpose(w_value, (0, 2, 3, 1)).reshape(blocks, local, rows)
    gate_t = jnp.transpose(w_gate, (0, 2, 3, 1)).reshape(blocks, local, rows)
    bf16, f32 = jnp.bfloat16, jnp.float32
    dma = pltpu.SemaphoreType.DMA
    vmem = pl.BlockSpec(memory_space=pltpu.VMEM)
    hbm = pl.BlockSpec(memory_space=pltpu.HBM)
    per_dp = n_tp // n_dp
    return pl.pallas_call(
        functools.partial(fused_kernel, n_tp, n_dp),
        out_shape=(
            pltpu.VMEM(resid.shape, resid.dtype),
            pltpu.VMEM(states.shape, states.dtype),
        ),
        in_specs=[vmem] * 4 + [hbm] * 6,
        out_specs=(vmem, vmem),
        scratch_shapes=[
            pltpu.VMEM(w_query.shape, bf16),
            pltpu.VMEM(w_forget.shape, bf16),
            pltpu.VMEM(value_t.shape, bf16),
            pltpu.VMEM(gate_t.shape, bf16),
            pltpu.VMEM((blocks, local, width), bf16),
            pltpu.VMEM((blocks, seqs, cols), bf16),
            pltpu.VMEM((blocks, n_dp, per_dp, seqs, cols), bf16),
            pltpu.VMEM((n_dp * seqs, rows), bf16),
            pltpu.VMEM((blocks, n_dp, 4, seqs, cols), bf16),
            pltpu.VMEM((blocks, n_dp, 4, seqs, cols), bf16),
            pltpu.VMEM((blocks, n_dp, 8, 128), f32),
            pltpu.VMEM((blocks, n_dp, 8, 128), f32),
            pltpu.VMEM((blocks, 2, seqs, cols), bf16),
            pltpu.VMEM((blocks, n_tp, 2, seqs, cols), bf16),
            pltpu.VMEM((heads, seqs, head_dim), f32),
            pltpu.VMEM((heads, seqs, head_dim), f32),
            pltpu.VMEM((heads, slice_cols, 128), f32),
            pltpu.VMEM((heads, slice_cols, 128), f32),
            pltpu.VMEM((blocks, heads * seqs // 128, 128), f32),
            pltpu.VMEM((blocks, n_tp, heads * seqs // 128, 128), f32),
            pltpu.VMEM((blocks, n_tp, seqs, cols), bf16),
            pltpu.VMEM((blocks, n_tp, seqs, cols), bf16),
            dma((blocks, 5)),
            dma((blocks,)),
            dma((blocks,)),
            dma((blocks, n_dp, per_dp)),
            dma((blocks, n_dp)),
            dma((blocks, n_dp)),
            dma((blocks, n_dp)),
            dma((blocks, n_dp)),
            dma((blocks,)),
            dma((blocks, n_tp)),
            dma((blocks,)),
            dma((blocks,)),
            dma((blocks,)),
            dma((blocks,)),
        ],
        compiler_params=pltpu.CompilerParams(
            collective_id=0, has_side_effects=True, vmem_limit_bytes=56 * 1024 * 1024
        ),
    )(
        resid,
        norm_gain,
        gate_floor,
        jnp.transpose(out_gain, (0, 2, 1)),
        w_query,
        w_forget,
        value_t,
        gate_t,
        w_out.reshape(blocks, local, width),
        states,
    )


def choose(n_tp, n_dp, *args):
    resid, w_query, states = args[0], args[2], args[7]
    seqs, cols = resid.shape
    _, _, heads, slice_cols, head_dim = states.shape
    whole_tiles = (
        cols == 128
        and head_dim == 128
        and heads == n_tp
        and slice_cols == 8
        and w_query.shape[2] == cols
        and heads * slice_cols == cols
        and n_tp % n_dp == 0
        and seqs % 16 == 0
        and seqs <= 128
        and heads * seqs % 128 == 0
        and heads * seqs >= 128
        and 1024 % seqs == 0
    )
    body = functools.partial(fused_shards, n_tp, n_dp) if whole_tiles else shards
    return body(*args)


def solution(mesh):
    return jax.shard_map(
        functools.partial(choose, mesh.shape["tp"], mesh.shape["dp"]),
        mesh=mesh,
        in_specs=(
            P("dp", "tp"),
            P(),
            P(None, "dp", "tp"),
            P(None, "dp", "tp"),
            P(None, "dp", None, "tp"),
            P(None, "dp", None, "tp"),
            P(),
            P(None, "dp", None, "tp", None),
            P(None, None, "tp"),
            P(None, None, "tp", None),
        ),
        out_specs=(P("dp", "tp"), P(None, "dp", None, "tp", None)),
        check_vma=False,
    )
```
